32 devices in a mesh: fs: 8 (over z, core), tp: 4 (over y, x).
Axes of the slice: x: 2, y: 2, z: 4, core: 2. Of those that a mesh axis runs over, the one named last changes fastest.
Arguments:
- in_saved: bfloat16 [6144, 2048], P(('fs', 'tp')), may hold values from -6 to 6
- in_cotangent: bfloat16 [6144, 2048], P(('fs', 'tp')), as said below
- point_saved: bfloat16 [6144, 2048], P(('fs', 'tp')), may hold values from -6 to 6
- point_cotangent: bfloat16 [6144, 2048], P(('fs', 'tp')), as said below
- in_basis: bfloat16 [2048, 128], replicated, as said below
- point_basis: bfloat16 [2048, 128], replicated, as said below
- in_first: float32 [128, 2048], P('fs', 'tp'), may hold values from -3 to 3
- in_second: float32 [128, 2048], P('fs', 'tp'), may hold values from 0.02 to 2
- point_first: float32 [128, 2048], P('fs', 'tp'), may hold values from -3 to 3
- point_second: float32 [128, 2048], P('fs', 'tp'), may hold values from 0.02 to 2
- in_master: float32 [2048, 2048], P('fs', 'tp'), may hold values from -3 to 3
- point_master: float32 [2048, 2048], P('fs', 'tp'), may hold values from -3 to 3
Outputs:
- in_first_new: float32 [128, 2048], P('fs', 'tp')
- in_second_new: float32 [128, 2048], P('fs', 'tp')
- point_first_new: float32 [128, 2048], P('fs', 'tp')
- point_second_new: float32 [128, 2048], P('fs', 'tp')
- in_step: float32 [2048, 2048], P('fs', 'tp')
- point_step: float32 [2048, 2048], P('fs', 'tp')
- in_master_new: float32 [2048, 2048], P('fs', 'tp')
- point_master_new: float32 [2048, 2048], P('fs', 'tp')
- in_copy: bfloat16 [2048, 2048], P(None, 'tp')
- point_copy: bfloat16 [2048, 2048], P(None, 'tp')
The draws below stay inside these ranges and needn't reach their ends.
Inputs may be any that keep to these rules, and one draw needn't show every extreme that they name: `in_cotangent`: real-valued entries of every column. `point_cotangent`: real-valued entries of every column. `in_basis`: real-valued basis of full rank. `point_basis`: real-valued basis of full rank.
All inputs are finite; a program needn't handle non-finite values.
Results may differ from the reference program's by a relative error of at most 0.0034.
Values may be sent and summed in bfloat16 or wider, within the bound.
A program may use at most 64 MiB of HBM per device.

```python
import math
import jax
import jax.numpy as jnp
from jax import lax

D = 2048
C = 2048
RANK = 128
TOK_DEV = 192
TOKENS = 6144
N_FS = 8
N_TP = 4


def cotangent_draw(key, width):
    keys = jax.random.split(jax.random.fold_in(key, 7), 3)
    offset = jax.random.uniform(keys[1], (width,), jnp.float32)
    levels = (jnp.arange(width).astype(jnp.float32) + offset) / width
    scales = 10.0 ** levels / 3.9
    shift = jax.random.randint(keys[2], (), 0, N_TP)
    device = jnp.arange(TOKENS) // TOK_DEV
    target = (device + shift) % N_TP
    column_block = jnp.arange(width) // (width // N_TP)
    boost = jnp.where(column_block[None, :] == target[:, None], 4.0, 1.0)
    noise = jax.random.truncated_normal(keys[0], -4.0, 4.0, (TOKENS, width), jnp.float32)
    return (noise * scales[None, :] * boost).astype(jnp.bfloat16)


def basis_draw(key, rows):
    keys = jax.random.split(jax.random.fold_in(key, 11), 2)
    offset = jax.random.uniform(keys[1], (RANK,), jnp.float32)
    levels = (jnp.arange(RANK).astype(jnp.float32) + offset) / RANK
    noise = jax.random.truncated_normal(keys[0], -4.0, 4.0, (rows, RANK), jnp.float32)
    scales = 10.0 ** levels
    return (noise * scales[None, :] / (3.9 * jnp.sqrt(rows * 1.0))).astype(jnp.bfloat16)


def draw_in_cotangent(key, part):
    return cotangent_draw(jax.random.fold_in(key, 1), C)


def draw_point_cotangent(key, part):
    return cotangent_draw(jax.random.fold_in(key, 2), D)


def draw_in_basis(key, part):
    return basis_draw(jax.random.fold_in(key, 3), D)


def draw_point_basis(key, part):
    return basis_draw(jax.random.fold_in(key, 4), C)


def shard_levels(rng, dims, cuts, smallest, largest):
    factor_of = 1.0
    for axis_at, parts in cuts:
        draws = jax.random.uniform(jax.random.fold_in(jax.random.fold_in(rng, 6), axis_at), (parts,), jnp.float32, smallest / len(cuts), largest / len(cuts))
        factor_of = factor_of * jnp.repeat(jnp.exp(draws), dims[axis_at] // parts).reshape((-1,) + (1,) * (len(dims) - 1 - axis_at))
    return factor_of


def normal_values(rng, dims, scale, most, shards=(), dtype=jnp.bfloat16):
    values = scale * jax.random.normal(rng, dims, jnp.float32)
    if shards:
        values = values * shard_levels(rng, dims, shards, -0.22, 0.18)
    return jnp.clip(values, -most, most).astype(dtype)


def setup_inputs(seed: int = 0) -> dict:
    seeds = jax.random.split(jax.random.key(seed), 13)
    in_saved = normal_values(seeds[0], (TOKENS, D), 1.0, 6.0, ((0, 32),))
    in_cotangent = draw_in_cotangent(jax.random.fold_in(seeds[12], 71), 0)
    point_saved = normal_values(seeds[2], (TOKENS, C), 1.0, 6.0, ((0, 32),))
    point_cotangent = draw_point_cotangent(jax.random.fold_in(seeds[12], 71), 0)
    in_basis = draw_in_basis(jax.random.fold_in(seeds[12], 71), 0)
    point_basis = draw_point_basis(jax.random.fold_in(seeds[12], 71), 0)
    in_first = normal_values(seeds[6], (RANK, C), 0.5, 3.0, ((0, 8), (1, 4)), jnp.float32)
    in_second = jnp.clip(jnp.exp(math.log(2.0) - 4.6051702 * jax.random.uniform(seeds[7], (RANK, C), jnp.float32) ** shard_levels(seeds[7], (RANK, C), ((0, 8), (1, 4)), -0.2, 0.2)), 0.02, 2.0)
    point_first = normal_values(seeds[8], (RANK, D), 0.5, 3.0, ((0, 8), (1, 4)), jnp.float32)
    point_second = jnp.clip(jnp.exp(math.log(2.0) - 4.6051702 * jax.random.uniform(seeds[9], (RANK, D), jnp.float32) ** shard_levels(seeds[9], (RANK, D), ((0, 8), (1, 4)), -0.2, 0.2)), 0.02, 2.0)
    in_master = normal_values(seeds[10], (D, C), 0.5, 3.0, ((0, 8), (1, 4)), jnp.float32)
    point_master = normal_values(seeds[11], (C, D), 0.5, 3.0, ((0, 8), (1, 4)), jnp.float32)
    return {"in_saved": in_saved, "in_cotangent": in_cotangent, "point_saved": point_saved, "point_cotangent": point_cotangent, "in_basis": in_basis, "point_basis": point_basis, "in_first": in_first, "in_second": in_second, "point_first": point_first, "point_second": point_second, "in_master": in_master, "point_master": point_master}


def low_grad(saved, cotangent, basis):
    basis_f = basis.astype(jnp.float32)
    saved_blocks = saved.reshape(N_FS, -1, saved.shape[1])
    cot_blocks = cotangent.reshape(N_FS, -1, cotangent.shape[1])

    def add_block(total, pair):
        reduced = jnp.dot(pair[0].astype(jnp.float32), basis_f).astype(jnp.bfloat16)
        term = jnp.dot(reduced.astype(jnp.float32).T, pair[1].astype(jnp.float32))
        return (total + term, None)
    start = jnp.zeros((basis.shape[1], cotangent.shape[1]), jnp.float32)
    total, unused = lax.scan(add_block, start, (saved_blocks, cot_blocks))
    return total

def moments(first, second, grad):
    first_new = 0.8 * first + 0.2 * grad
    second_new = 0.9 * second + 0.1 * grad * grad
    return (first_new, second_new, first_new / (jnp.sqrt(second_new) + 1e-08))

def reference(in_saved, in_cotangent, point_saved, point_cotangent, in_basis, point_basis, in_first, in_second, point_first, point_second, in_master, point_master):
    in_low = low_grad(in_saved, in_cotangent, in_basis)
    point_low = low_grad(point_saved, point_cotangent, point_basis)
    entries = 1.0 * in_low.shape[0] * (in_low.shape[1] + point_low.shape[1])
    squares = jnp.sum(in_low * in_low) + jnp.sum(point_low * point_low)
    rms_value = jnp.sqrt(squares / entries + 1e-06)
    clip_factor = jnp.minimum(1.0, 1.0 / rms_value)
    in_first_new, in_second_new, in_direction = moments(in_first, in_second, clip_factor * in_low)
    point_first_new, point_second_new, point_direction = moments(point_first, point_second, clip_factor * point_low)
    in_step = -jnp.dot(in_basis.astype(jnp.float32), in_direction, precision=lax.Precision.HIGHEST)
    point_step = -jnp.dot(point_basis.astype(jnp.float32), point_direction, precision=lax.Precision.HIGHEST)
    in_master_new = in_master + in_step
    point_master_new = point_master + point_step
    return (in_first_new, in_second_new, point_first_new, point_second_new, in_step, point_step, in_master_new, point_master_new, in_master_new.astype(jnp.bfloat16), point_master_new.astype(jnp.bfloat16))
```

```python
import functools

import jax
import jax.numpy as jnp
from jax import lax
from jax.experimental import pallas as pl
from jax.experimental.pallas import tpu as pltpu
from jax.sharding import PartitionSpec as P


def low_term(saved, cotangent, basis):
    reduced = jnp.dot(saved, basis, preferred_element_type=jnp.float32).astype(jnp.bfloat16)
    return lax.dot_general(
        reduced, cotangent, (((0,), (0,)), ((), ())), preferred_element_type=jnp.float32
    )


def moments(first, second, grad):
    first_new = 0.8 * first + 0.2 * grad
    second_new = 0.9 * second + 0.1 * grad * grad
    return (first_new, second_new, first_new / (jnp.sqrt(second_new) + 1e-08))


def weight_step(basis, direction, fs_count):
    row_count = basis.shape[0] // fs_count
    rows_here = lax.dynamic_slice_in_dim(basis, lax.axis_index("fs") * row_count, row_count, 0)
    return -jnp.dot(rows_here.astype(jnp.float32), direction, precision=lax.Precision.HIGHEST)


def body(
    in_saved,
    in_cotangent,
    point_saved,
    point_cotangent,
    in_basis,
    point_basis,
    in_first,
    in_second,
    point_first,
    point_second,
    in_master,
    point_master,
):
    fs_count = lax.axis_size("fs")
    in_low = low_term(in_saved, in_cotangent, in_basis)
    point_low = low_term(point_saved, point_cotangent, point_basis)
    rank_rows = in_low.shape[0]
    entries = 1.0 * rank_rows * (in_low.shape[1] + point_low.shape[1])
    part_in, part_point = (
        lax.psum_scatter(in_low, "tp", scatter_dimension=1, tiled=True),
        lax.psum_scatter(point_low, "tp", scatter_dimension=1, tiled=True),
    )
    sum_in, sum_point = lax.psum((part_in, part_point), "fs")
    squares = lax.psum(jnp.sum(sum_in * sum_in) + jnp.sum(sum_point * sum_point), "tp")
    clip_factor = jnp.minimum(1.0, 1.0 / jnp.sqrt(squares / entries + 1e-06))
    previous = (
        lax.all_gather(in_first, "fs", axis=0, tiled=True),
        lax.all_gather(in_second, "fs", axis=0, tiled=True),
        lax.all_gather(point_first, "fs", axis=0, tiled=True),
        lax.all_gather(point_second, "fs", axis=0, tiled=True),
    )
    in_first_all, in_second_all, in_direction = moments(
        previous[0], previous[1], clip_factor * sum_in
    )
    point_first_all, point_second_all, point_direction = moments(
        previous[2], previous[3], clip_factor * sum_point
    )
    row_count = rank_rows // fs_count
    row_start = lax.axis_index("fs") * row_count
    in_first_new = lax.dynamic_slice_in_dim(in_first_all, row_start, row_count, 0)
    in_second_new = lax.dynamic_slice_in_dim(in_second_all, row_start, row_count, 0)
    point_first_new = lax.dynamic_slice_in_dim(point_first_all, row_start, row_count, 0)
    point_second_new = lax.dynamic_slice_in_dim(point_second_all, row_start, row_count, 0)
    in_step = weight_step(in_basis, in_direction, fs_count)
    point_step = weight_step(point_basis, point_direction, fs_count)
    in_master_new = in_master + in_step
    point_master_new = point_master + point_step
    in_copy, point_copy = (
        lax.all_gather(in_master_new.astype(jnp.bfloat16), "fs", axis=0, tiled=True),
        lax.all_gather(point_master_new.astype(jnp.bfloat16), "fs", axis=0, tiled=True),
    )
    return (
        in_first_new,
        in_second_new,
        point_first_new,
        point_second_new,
        in_step,
        point_step,
        in_master_new,
        point_master_new,
        in_copy,
        point_copy,
    )


MESH = pl.DeviceIdType.MESH
HBM = pl.BlockSpec(memory_space=pl.ANY)
WHOLE = pl.BlockSpec(memory_space=pltpu.VMEM)


def exchange_kernel(
    n_fs,
    n_tp,
    in_saved,
    in_cot,
    point_saved,
    point_cot,
    in_basis,
    point_basis,
    in_first,
    in_second,
    point_first,
    point_second,
    in_master,
    point_master,
    dirs_out,
    moments_out,
    gathered_out,
    saved,
    cot,
    basis,
    master,
    part,
    mate,
    tp_got,
    fs_got,
    total,
    dirs,
    gathered,
    scalars,
    load_sem,
    out_sem,
    mate_sems,
    tp_sems,
    fs_sems,
    tp_scalar_sems,
    fs_scalar_sems,
    dir_sems,
    dir_mate_sems,
    ring_sems,
    ring_mate_sems,
):
    f, t = lax.axis_index("fs"), lax.axis_index("tp")
    z, core = f // 2, f % 2
    n_z = n_fs // 2
    mate_f = f + 1 - 2 * core
    width = in_first.shape[1]
    rows = in_first.shape[0]

    def at_z(step):
        return lax.rem(z + step + n_z, n_z)

    def at_tp(step):
        return lax.rem(t + step + n_tp, n_tp)

    def at_fs(step):
        return lax.rem(f + step + n_fs, n_fs)

    def remote(src, dst, sems, index, device):
        return pltpu.make_async_remote_copy(
            src_ref=src,
            dst_ref=dst,
            send_sem=sems.at[(0, *index)],
            recv_sem=sems.at[(1, *index)],
            device_id=device,
            device_id_type=MESH,
        )

    loads = []
    sources = (
        (in_master, master.at[0]),
        (point_master, master.at[1]),
        (in_basis, basis.at[0]),
        (in_saved, saved.at[0]),
        (in_cot, cot.at[0]),
        (point_basis, basis.at[1]),
        (point_saved, saved.at[1]),
        (point_cot, cot.at[1]),
    )
    for k, (src, dst) in enumerate(sources):
        copy = pltpu.make_async_copy(src, dst, load_sem.at[k])
        copy.start()
        loads.append(copy)

    barrier = pltpu.get_barrier_semaphore()
    for step in range(1, n_fs):
        pl.semaphore_signal(barrier, inc=1, device_id=(at_fs(step), t), device_id_type=MESH)
    for step in range(1, n_tp):
        pl.semaphore_signal(barrier, inc=1, device_id=(f, at_tp(step)), device_id_type=MESH)

    sends = []
    outs = []

    def put_out(m, order, slot):
        copy = pltpu.make_async_copy(
            gathered.at[m, slot], gathered_out.at[m, slot], out_sem.at[m, order]
        )
        copy.start()
        outs.append(copy)

    def ring_send(step):
        for m in range(2):
            slot = 2 * at_z(-step if m == 0 else step) + core
            copy = remote(
                gathered.at[m, slot],
                gathered.at[m, slot],
                ring_sems,
                (m, step),
                (2 * at_z(1 if m == 0 else -1) + core, t),
            )
            copy.start()
            sends.append(copy)

    def mate_send(step):
        for m in range(2):
            slot = 2 * at_z(-step if m == 0 else step) + core
            copy = remote(
                gathered.at[m, slot], gathered.at[m, slot], ring_mate_sems, (m, step), (mate_f, t)
            )
            copy.start()
            sends.append(copy)
            put_out(m, step, slot)

    def ring_wait(step):
        for m in range(2):
            slot = 2 * at_z(-step - 1 if m == 0 else step + 1) + core
            remote(
                gathered.at[m, slot], gathered.at[m, slot], ring_sems, (m, step), (f, t)
            ).wait_recv()

    def ring_advance(step):
        ring_wait(step - 1)
        if step < n_z - 1:
            ring_send(step)
        mate_send(step)

    for m in range(2):
        loads[m].wait()
        gathered[m, f] = master[m].astype(jnp.bfloat16)
    pl.semaphore_wait(barrier, n_fs + n_tp - 2)
    ring_send(0)
    mate_send(0)

    for m in range(2):
        for k in range(3):
            loads[2 + 3 * m + k].wait()
        reduced = jnp.dot(saved[m], basis[m], preferred_element_type=jnp.float32).astype(
            jnp.bfloat16
        )
        for k in range(n_tp):
            low = lax.dot_general(
                reduced,
                cot[m, :, k * width : (k + 1) * width],
                (((0,), (0,)), ((), ())),
                preferred_element_type=jnp.float32,
            )
            for g in range(n_fs):
                part[m, g % 2, k, g // 2] = low[g * rows : (g + 1) * rows]
        copy = remote(part.at[m, 1 - core], mate.at[m], mate_sems, (m,), (mate_f, t))
        copy.start()
        sends.append(copy)

    for m in range(2):
        remote(mate.at[m], mate.at[m], mate_sems, (m,), (mate_f, t)).wait_recv()
        for step in range(1, n_tp + 1):
            to = at_tp(step) if step < n_tp else t
            part[m, core, to] = part[m, core, to] + mate[m, to]
            if step < n_tp:
                copy = remote(
                    part.at[m, core, to], tp_got.at[m, step - 1], tp_sems, (m, step - 1), (f, to)
                )
                copy.start()
                sends.append(copy)
    ring_advance(1)

    for m in range(2):
        for step in range(1, n_tp):
            remote(
                tp_got.at[m, step - 1], tp_got.at[m, step - 1], tp_sems, (m, step - 1), (f, t)
            ).wait_recv()
        for step in range(1, n_z + 1):
            to = at_z(step) if step < n_z else z
            value = part[m, core, t, to]
            for k in range(n_tp - 1):
                value = value + tp_got[m, k, to]
            total[m, to] = value
            if step < n_z:
                copy = remote(
                    total.at[m, to],
                    fs_got.at[m, step - 1],
                    fs_sems,
                    (m, step - 1),
                    (2 * to + core, t),
                )
                copy.start()
                sends.append(copy)
    grads = []
    for m in range(2):
        value = total[m, z]
        for step in range(1, n_z):
            remote(
                fs_got.at[m, step - 1], fs_got.at[m, step - 1], fs_sems, (m, step - 1), (f, t)
            ).wait_recv()
            value = value + fs_got[m, step - 1]
        grads.append(value)

    def add_scalars(value, count, base, sems, device):
        scalars[base] = jnp.broadcast_to(value, scalars.shape[1:])
        for step in range(1, count):
            copy = remote(
                scalars.at[base], scalars.at[base + step], sems, (step - 1,), device(step)
            )
            copy.start()
            sends.append(copy)
        result = scalars[base]
        for step in range(1, count):
            slot = scalars.at[base + step]
            remote(slot, slot, sems, (step - 1,), (f, t)).wait_recv()
            result = result + scalars[base + step]
        return result[0:1, 0:1]

    squares = jnp.sum(grads[0] * grads[0] + grads[1] * grads[1], keepdims=True)
    squares = add_scalars(squares, n_tp, 0, tp_scalar_sems, lambda step: (f, at_tp(step)))
    squares = add_scalars(squares, n_fs, n_tp, fs_scalar_sems, lambda step: (at_fs(step), t))
    entries = 2.0 * rows * n_fs * width * n_tp
    clip = jnp.minimum(1.0, 1.0 / jnp.sqrt(squares / entries + 1e-06))

    old = ((in_first, in_second), (point_first, point_second))
    for m in range(2):
        first, second, direction = moments(old[m][0][...], old[m][1][...], clip * grads[m])
        moments_out[2 * m] = first
        moments_out[2 * m + 1] = second
        dirs[f, m] = direction
    for step in range(1, n_z):
        copy = remote(
            dirs.at[f], dirs.at[f], dir_sems, (step - 1,), (2 * at_z(step) + core, t)
        )
        copy.start()
        sends.append(copy)

    def dir_mate(step):
        slot = 2 * at_z(-step) + core
        copy = remote(dirs.at[slot], dirs.at[slot], dir_mate_sems, (step,), (mate_f, t))
        copy.start()
        sends.append(copy)

    dir_mate(0)
    for step in range(1, n_z):
        slot = 2 * at_z(-step) + core
        remote(dirs.at[slot], dirs.at[slot], dir_sems, (step - 1,), (f, t)).wait_recv()
        dir_mate(step)
    for step in range(2, n_z):
        ring_advance(step)
    for step in range(n_z):
        slot = 2 * at_z(-step) + 1 - core
        remote(dirs.at[slot], dirs.at[slot], dir_mate_sems, (step,), (f, t)).wait_recv()
        for m in range(2):
            slot = 2 * at_z(-step if m == 0 else step) + 1 - core
            remote(
                gathered.at[m, slot], gathered.at[m, slot], ring_mate_sems, (m, step), (f, t)
            ).wait_recv()
            put_out(m, n_z + step, slot)
    dirs_out[...] = dirs[...]
    for copy in sends:
        copy.wait_send()
    for copy in outs:
        copy.wait()


def exchange(n_fs, n_tp, *args):
    saved, basis, first, master = args[0], args[4], args[6], args[10]
    rows, width = first.shape
    n_z = n_fs // 2
    f32, bf16 = jnp.float32, jnp.bfloat16
    dma = pltpu.SemaphoreType.DMA
    return pl.pallas_call(
        functools.partial(exchange_kernel, n_fs, n_tp),
        out_shape=(
            jax.ShapeDtypeStruct((n_fs, 2, rows, width), f32),
            jax.ShapeDtypeStruct((4, rows, width), f32),
            jax.ShapeDtypeStruct((2, n_fs, *master.shape), bf16),
        ),
        in_specs=[HBM] * 6 + [WHOLE] * 4 + [HBM] * 2,
        out_specs=(WHOLE, WHOLE, HBM),
        scratch_shapes=[
            pltpu.VMEM((2, *saved.shape), bf16),
            pltpu.VMEM((2, *args[1].shape), bf16),
            pltpu.VMEM((2, *basis.shape), bf16),
            pltpu.VMEM((2, *master.shape), f32),
            pltpu.VMEM((2, 2, n_tp, n_z, rows, width), f32),
            pltpu.VMEM((2, n_tp, n_z, rows, width), f32),
            pltpu.VMEM((2, n_tp - 1, n_z, rows, width), f32),
            pltpu.VMEM((2, n_z - 1, rows, width), f32),
            pltpu.VMEM((2, n_z, rows, width), f32),
            pltpu.VMEM((n_fs, 2, rows, width), f32),
            pltpu.VMEM((2, n_fs, *master.shape), bf16),
            pltpu.VMEM((n_tp + n_fs, 8, 128), f32),
            dma((8,)),
            dma((2, n_fs)),
            dma((2, 2)),
            dma((2, 2, n_tp - 1)),
            dma((2, 2, n_z - 1)),
            dma((2, n_tp - 1)),
            dma((2, n_fs - 1)),
            dma((2, n_z - 1)),
            dma((2, n_z)),
            dma((2, 2, n_z - 1)),
            dma((2, 2, n_z)),
        ],
        compiler_params=pltpu.CompilerParams(
            collective_id=0, has_side_effects=True, vmem_limit_bytes=48 * 2**20
        ),
        name="exchange",
    )(*args)


def update_kernel(
    dirs,
    moments_new,
    in_basis,
    point_basis,
    in_gathered,
    point_gathered,
    in_master,
    point_master,
    in_first_new,
    in_second_new,
    point_first_new,
    point_second_new,
    in_step,
    point_step,
    in_master_new,
    point_master_new,
    in_copy,
    point_copy,
    split,
):
    i = pl.program_id(0)
    f = lax.axis_index("fs")
    rank = split.shape[1] // 2

    @pl.when(i == 0)
    def first_tile():
        for m in range(2):
            whole = dirs[:, m].reshape(rank, split.shape[2])
            high = whole.astype(jnp.bfloat16)
            split[m, :rank] = high
            split[m, rank:] = (whole - high.astype(jnp.float32)).astype(jnp.bfloat16)
        for k, out in enumerate(
            (in_first_new, in_second_new, point_first_new, point_second_new)
        ):
            out[...] = moments_new[k]

    groups = (
        (in_basis, in_gathered, in_master, in_step, in_master_new, in_copy),
        (point_basis, point_gathered, point_master, point_step, point_master_new, point_copy),
    )
    for m, (basis, gathered, master, step, master_new, copy) in enumerate(groups):
        twice = jnp.concatenate([basis[...], basis[...]], axis=1)
        move = -jnp.dot(twice, split[m], preferred_element_type=jnp.float32)
        copy[...] = (gathered[0, 0].astype(jnp.float32) + move).astype(jnp.bfloat16)

        @pl.when(i == f)
        def own_tile():
            step[...] = move
            new = master[...] + move
            master_new[...] = new
            copy[...] = new.astype(jnp.bfloat16)


def update(n_fs, dirs, moments_new, gathered, *args):
    in_basis, in_first, in_master = args[4], args[6], args[10]
    row_count, width = in_master.shape
    rank = in_basis.shape[1]
    f32, bf16 = jnp.float32, jnp.bfloat16

    def fixed(shape):
        return pl.BlockSpec(shape, lambda i: (0,) * len(shape))

    tile = pl.BlockSpec((row_count, rank), lambda i: (i, 0))
    copy_tile = pl.BlockSpec((row_count, width), lambda i: (i, 0))

    def gathered_tile(m):
        return pl.BlockSpec((1, 1, row_count, width), lambda i: (m, i, 0, 0))

    return pl.pallas_call(
        update_kernel,
        grid=(n_fs,),
        out_shape=(
            *(jax.ShapeDtypeStruct(in_first.shape, f32),) * 4,
            *(jax.ShapeDtypeStruct(in_master.shape, f32),) * 4,
            *(jax.ShapeDtypeStruct((row_count * n_fs, width), bf16),) * 2,
        ),
        in_specs=[
            fixed(dirs.shape),
            fixed(moments_new.shape),
            tile,
            tile,
            gathered_tile(0),
            gathered_tile(1),
            fixed(in_master.shape),
            fixed(in_master.shape),
        ],
        out_specs=(
            *(fixed(in_first.shape),) * 4,
            *(fixed(in_master.shape),) * 4,
            copy_tile,
            copy_tile,
        ),
        scratch_shapes=[pltpu.VMEM((2, 2 * rank, width), bf16)],
        compiler_params=pltpu.CompilerParams(vmem_limit_bytes=32 * 2**20),
        name="update",
    )(dirs, moments_new, in_basis, args[5], gathered, gathered, in_master, args[11])


def fused_body(*args):
    n_fs, n_tp = lax.axis_size("fs"), lax.axis_size("tp")
    dirs, moments_new, gathered = exchange(n_fs, n_tp, *args)
    return update(n_fs, dirs, moments_new, gathered, *args)


def pick_body(*args):
    n_fs, n_tp = lax.axis_size("fs"), lax.axis_size("tp")
    first = args[6]
    fits = n_fs % 2 == 0 and n_fs > 2 and n_tp > 1
    if fits and first.shape[0] % 16 == 0 and first.shape[1] % 128 == 0:
        return fused_body(*args)
    return body(*args)


def solution(mesh):
    return jax.shard_map(
        pick_body,
        mesh=mesh,
        in_specs=(
            P(("fs", "tp"), None),
            P(("fs", "tp"), None),
            P(("fs", "tp"), None),
            P(("fs", "tp"), None),
            P(),
            P(),
            P("fs", "tp"),
            P("fs", "tp"),
            P("fs", "tp"),
            P("fs", "tp"),
            P("fs", "tp"),
            P("fs", "tp"),
        ),
        out_specs=(
            P("fs", "tp"),
            P("fs", "tp"),
            P("fs", "tp"),
            P("fs", "tp"),
            P("fs", "tp"),
            P("fs", "tp"),
            P("fs", "tp"),
            P("fs", "tp"),
            P(None, "tp"),
            P(None, "tp"),
        ),
        check_vma=False,
    )
```

```python
import functools

import jax
import jax.numpy as jnp
from jax import lax
from jax.experimental import pallas as pl
from jax.experimental.pallas import tpu as pltpu
from jax.sharding import PartitionSpec as P


def low_term(saved, cotangent, basis):
    reduced = jnp.dot(saved, basis, preferred_element_type=jnp.float32).astype(jnp.bfloat16)
    return lax.dot_general(
        reduced, cotangent, (((0,), (0,)), ((), ())), preferred_element_type=jnp.float32
    )


def moments(first, second, grad):
    first_new = 0.8 * first + 0.2 * grad
    second_new = 0.9 * second + 0.1 * grad * grad
    return (first_new, second_new, first_new / (jnp.sqrt(second_new) + 1e-08))


def weight_step(basis, direction, fs_count):
    row_count = basis.shape[0] // fs_count
    rows_here = lax.dynamic_slice_in_dim(basis, lax.axis_index("fs") * row_count, row_count, 0)
    return -jnp.dot(rows_here.astype(jnp.float32), direction, precision=lax.Precision.HIGHEST)


def body(
    in_saved,
    in_cotangent,
    point_saved,
    point_cotangent,
    in_basis,
    point_basis,
    in_first,
    in_second,
    point_first,
    point_second,
    in_master,
    point_master,
):
    fs_count = lax.axis_size("fs")
    in_low = low_term(in_saved, in_cotangent, in_basis)
    point_low = low_term(point_saved, point_cotangent, point_basis)
    rank_rows = in_low.shape[0]
    entries = 1.0 * rank_rows * (in_low.shape[1] + point_low.shape[1])
    part_in, part_point = (
        lax.psum_scatter(in_low, "tp", scatter_dimension=1, tiled=True),
        lax.psum_scatter(point_low, "tp", scatter_dimension=1, tiled=True),
    )
    sum_in, sum_point = lax.psum((part_in, part_point), "fs")
    squares = lax.psum(jnp.sum(sum_in * sum_in) + jnp.sum(sum_point * sum_point), "tp")
    clip_factor = jnp.minimum(1.0, 1.0 / jnp.sqrt(squares / entries + 1e-06))
    previous = (
        lax.all_gather(in_first, "fs", axis=0, tiled=True),
        lax.all_gather(in_second, "fs", axis=0, tiled=True),
        lax.all_gather(point_first, "fs", axis=0, tiled=True),
        lax.all_gather(point_second, "fs", axis=0, tiled=True),
    )
    in_first_all, in_second_all, in_direction = moments(
        previous[0], previous[1], clip_factor * sum_in
    )
    point_first_all, point_second_all, point_direction = moments(
        previous[2], previous[3], clip_factor * sum_point
    )
    row_count = rank_rows // fs_count
    row_start = lax.axis_index("fs") * row_count
    in_first_new = lax.dynamic_slice_in_dim(in_first_all, row_start, row_count, 0)
    in_second_new = lax.dynamic_slice_in_dim(in_second_all, row_start, row_count, 0)
    point_first_new = lax.dynamic_slice_in_dim(point_first_all, row_start, row_count, 0)
    point_second_new = lax.dynamic_slice_in_dim(point_second_all, row_start, row_count, 0)
    in_step = weight_step(in_basis, in_direction, fs_count)
    point_step = weight_step(point_basis, point_direction, fs_count)
    in_master_new = in_master + in_step
    point_master_new = point_master + point_step
    in_copy, point_copy = (
        lax.all_gather(in_master_new.astype(jnp.bfloat16), "fs", axis=0, tiled=True),
        lax.all_gather(point_master_new.astype(jnp.bfloat16), "fs", axis=0, tiled=True),
    )
    return (
        in_first_new,
        in_second_new,
        point_first_new,
        point_second_new,
        in_step,
        point_step,
        in_master_new,
        point_master_new,
        in_copy,
        point_copy,
    )


MESH = pl.DeviceIdType.MESH
HBM = pl.BlockSpec(memory_space=pl.ANY)
VMEM_BYTES = 67_043_328
WHOLE = pl.BlockSpec(memory_space=pltpu.VMEM)


def exchange_kernel(
    n_fs,
    n_tp,
    in_saved,
    in_cot,
    point_saved,
    point_cot,
    in_basis,
    point_basis,
    in_first,
    in_second,
    point_first,
    point_second,
    in_master,
    point_master,
    dirs_out,
    moments_out,
    gathered_out,
    saved,
    cot,
    basis,
    master,
    part,
    mate,
    tp_put,
    tp_got,
    fs_got,
    total,
    dirs,
    old,
    gathered,
    scalars,
    load_sem,
    out_sem,
    mate_sems,
    tp_sems,
    fs_sems,
    tp_scalar_sems,
    fs_scalar_sems,
    dir_sems,
    dir_mate_sems,
    ring_sems,
    ring_mate_sems,
):
    f, t = lax.axis_index("fs"), lax.axis_index("tp")
    z, core = f // 2, f % 2
    n_z = n_fs // 2
    mate_f = f + 1 - 2 * core
    width = in_first.shape[1]
    rows = in_first.shape[0]

    def at_z(step):
        return lax.rem(z + step + n_z, n_z)

    def at_tp(step):
        return lax.rem(t + step + n_tp, n_tp)

    def at_fs(step):
        return lax.rem(f + step + n_fs, n_fs)

    def remote(src, dst, sems, index, device):
        return pltpu.make_async_remote_copy(
            src_ref=src,
            dst_ref=dst,
            send_sem=sems.at[(0, *index)],
            recv_sem=sems.at[(1, *index)],
            device_id=device,
            device_id_type=MESH,
        )

    loads = []
    sources = (
        (in_master, master.at[0]),
        (point_master, master.at[1]),
        (in_basis, basis.at[0]),
        (in_saved, saved.at[0]),
        (in_cot, cot.at[0]),
        (point_basis, basis.at[1]),
        (point_saved, saved.at[1]),
        (point_cot, cot.at[1]),
        (in_first, old.at[0]),
        (in_second, old.at[1]),
        (point_first, old.at[2]),
        (point_second, old.at[3]),
    )
    for k, (src, dst) in enumerate(sources):
        copy = pltpu.make_async_copy(src, dst, load_sem.at[k])
        copy.start()
        loads.append(copy)

    barrier = pltpu.get_barrier_semaphore()
    for step in range(1, n_fs):
        pl.semaphore_signal(barrier, inc=1, device_id=(at_fs(step), t), device_id_type=MESH)
    for step in range(1, n_tp):
        pl.semaphore_signal(barrier, inc=1, device_id=(f, at_tp(step)), device_id_type=MESH)

    sends = []

    def out_copy(m, slot):
        return pltpu.make_async_copy(
            gathered.at[m, slot], gathered_out.at[m, slot], out_sem.at[m, slot]
        )

    def mate_copy(m, slot, sem):
        return remote(
            gathered.at[m, slot], gathered.at[m, slot], ring_mate_sems, (m, sem), (mate_f, t)
        )

    def line_copy(d, m, step):
        slot = 2 * (z - step if d == 0 else z + step) + core
        to = z + 1 if d == 0 else z - 1
        return remote(
            gathered.at[m, slot], gathered.at[m, slot], ring_sems, (d, m, step), (2 * to + core, t)
        )

    def line_sends(d, step):
        if d == 0:
            return (z >= step) & (z + 1 < n_z)
        return (z + step < n_z) & (z >= 1)

    def line_start(m, step):
        for d in range(2):

            @pl.when(line_sends(d, step))
            def start():
                line_copy(d, m, step).start()

    def line_relay(m, step):
        for d in range(2):
            owner = z - 1 - step if d == 0 else z + 1 + step

            @pl.when((owner >= 0) & (owner < n_z))
            def arrived():
                slot = 2 * owner + core
                remote(
                    gathered.at[m, slot], gathered.at[m, slot], ring_sems, (d, m, step), (f, t)
                ).wait_recv()
                if step + 1 < n_z - 1:

                    @pl.when(line_sends(d, step + 1))
                    def onward():
                        line_copy(d, m, step + 1).start()

                mate_copy(m, slot, owner).start()
                out_copy(m, slot).start()

    for m in range(2):
        loads[m].wait()
        gathered[m, f] = master[m].astype(jnp.bfloat16)
    pl.semaphore_wait(barrier, n_fs + n_tp - 2)
    for m in range(2):
        line_start(m, 0)
    for m in range(2):
        mate_copy(m, f, z).start()
        out_copy(m, f).start()
    relays = [(m, step) for step in range(n_z - 1) for m in range(2)]

    for m in range(2):
        for k in range(3):
            loads[2 + 3 * m + k].wait()
        reduced = jnp.dot(saved[m], basis[m], preferred_element_type=jnp.float32).astype(
            jnp.bfloat16
        )
        for k in range(n_tp):
            low = lax.dot_general(
                reduced,
                cot[m, :, k * width : (k + 1) * width],
                (((0,), (0,)), ((), ())),
                preferred_element_type=jnp.float32,
            )
            for g in range(n_fs):
                part[m, g % 2, k, g // 2] = low[g * rows : (g + 1) * rows]
        copy = remote(part.at[m, 1 - core], mate.at[m], mate_sems, (m,), (mate_f, t))
        copy.start()
        sends.append(copy)

    for m in range(2):
        remote(mate.at[m], mate.at[m], mate_sems, (m,), (mate_f, t)).wait_recv()
        for step in range(1, n_tp + 1):
            to = at_tp(step) if step < n_tp else t
            value = part[m, core, to] + mate[m, to]
            if step == n_tp:
                part[m, core, to] = value
            else:
                tp_put[m, step - 1] = value.astype(jnp.bfloat16)
                copy = remote(
                    tp_put.at[m, step - 1], tp_got.at[m, step - 1], tp_sems, (m, step - 1), (f, to)
                )
                copy.start()
                sends.append(copy)
    line_relay(*relays[0])

    for m in range(2):
        for step in range(1, n_tp):
            remote(
                tp_got.at[m, step - 1], tp_got.at[m, step - 1], tp_sems, (m, step - 1), (f, t)
            ).wait_recv()
        for step in range(1, n_z + 1):
            to = at_z(step) if step < n_z else z
            value = part[m, core, t, to]
            for k in range(n_tp - 1):
                value = value + tp_got[m, k, to].astype(jnp.float32)
            total[m, to] = value
            if step < n_z:
                copy = remote(
                    total.at[m, to],
                    fs_got.at[m, step - 1],
                    fs_sems,
                    (m, step - 1),
                    (2 * to + core, t),
                )
                copy.start()
                sends.append(copy)
    line_relay(*relays[1])
    grads = []
    for m in range(2):
        value = total[m, z]
        for step in range(1, n_z):
            remote(
                fs_got.at[m, step - 1], fs_got.at[m, step - 1], fs_sems, (m, step - 1), (f, t)
            ).wait_recv()
            value = value + fs_got[m, step - 1]
        grads.append(value)

    def add_scalars(value, count, base, sems, device):
        scalars[base] = jnp.broadcast_to(value, scalars.shape[1:])
        for step in range(1, count):
            copy = remote(
                scalars.at[base], scalars.at[base + step], sems, (step - 1,), device(step)
            )
            copy.start()
            sends.append(copy)
        result = scalars[base]
        for step in range(1, count):
            slot = scalars.at[base + step]
            remote(slot, slot, sems, (step - 1,), (f, t)).wait_recv()
            result = result + scalars[base + step]
        return result[0:1, 0:1]

    line_relay(*relays[2])
    squares = jnp.sum(grads[0] * grads[0] + grads[1] * grads[1], keepdims=True)
    squares = add_scalars(squares, n_tp, 0, tp_scalar_sems, lambda step: (f, at_tp(step)))
    squares = add_scalars(squares, n_fs, n_tp, fs_scalar_sems, lambda step: (at_fs(step), t))
    line_relay(*relays[3])
    entries = 2.0 * rows * n_fs * width * n_tp
    clip = jnp.minimum(1.0, 1.0 / jnp.sqrt(squares / entries + 1e-06))

    for copy in loads[8:]:
        copy.wait()
    for m in range(2):
        first, second, direction = moments(old[2 * m], old[2 * m + 1], clip * grads[m])
        moments_out[2 * m] = first
        moments_out[2 * m + 1] = second
        dirs[f, m] = direction
    for step in range(1, n_z):
        copy = remote(
            dirs.at[f], dirs.at[f], dir_sems, (step - 1,), (2 * at_z(step) + core, t)
        )
        copy.start()
        sends.append(copy)

    def dir_mate(step):
        slot = 2 * at_z(-step) + core
        copy = remote(dirs.at[slot], dirs.at[slot], dir_mate_sems, (step,), (mate_f, t))
        copy.start()
        sends.append(copy)

    dir_mate(0)
    for step in range(1, n_z):
        slot = 2 * at_z(-step) + core
        remote(dirs.at[slot], dirs.at[slot], dir_sems, (step - 1,), (f, t)).wait_recv()
        dir_mate(step)
    for m, step in relays[4:]:
        line_relay(m, step)
    for step in range(n_z):
        slot = 2 * at_z(-step) + 1 - core
        remote(dirs.at[slot], dirs.at[slot], dir_mate_sems, (step,), (f, t)).wait_recv()
    dirs_out[...] = dirs[...]
    for m in range(2):
        for owner in range(n_z):
            slot = 2 * owner + 1 - core
            mate_copy(m, slot, owner).wait_recv()
            out_copy(m, slot).start()
    for copy in sends:
        copy.wait_send()
    for m in range(2):
        for owner in range(n_z):
            mate_copy(m, 2 * owner + core, owner).wait_send()
        for slot in range(n_fs):
            out_copy(m, slot).wait()
        for step in range(n_z - 1):
            for d in range(2):

                @pl.when(line_sends(d, step))
                def sent():
                    line_copy(d, m, step).wait_send()


def exchange(n_fs, n_tp, *args):
    saved, basis, first, master = args[0], args[4], args[6], args[10]
    rows, width = first.shape
    n_z = n_fs // 2
    f32, bf16 = jnp.float32, jnp.bfloat16
    dma = pltpu.SemaphoreType.DMA
    return pl.pallas_call(
        functools.partial(exchange_kernel, n_fs, n_tp),
        out_shape=(
            jax.ShapeDtypeStruct((n_fs, 2, rows, width), f32),
            jax.ShapeDtypeStruct((4, rows, width), f32),
            jax.ShapeDtypeStruct((2, n_fs, *master.shape), bf16),
        ),
        in_specs=[HBM] * 12,
        out_specs=(WHOLE, WHOLE, HBM),
        scratch_shapes=[
            pltpu.VMEM((2, *saved.shape), bf16),
            pltpu.VMEM((2, *args[1].shape), bf16),
            pltpu.VMEM((2, *basis.shape), bf16),
            pltpu.VMEM((2, *master.shape), f32),
            pltpu.VMEM((2, 2, n_tp, n_z, rows, width), f32),
            pltpu.VMEM((2, n_tp, n_z, rows, width), f32),
            pltpu.VMEM((2, n_tp - 1, n_z, rows, width), bf16),
            pltpu.VMEM((2, n_tp - 1, n_z, rows, width), bf16),
            pltpu.VMEM((2, n_z - 1, rows, width), f32),
            pltpu.VMEM((2, n_z, rows, width), f32),
            pltpu.VMEM((n_fs, 2, rows, width), f32),
            pltpu.VMEM((4, rows, width), f32),
            pltpu.VMEM((2, n_fs, *master.shape), bf16),
            pltpu.VMEM((n_tp + n_fs, 8, 128), f32),
            dma((12,)),
            dma((2, n_fs)),
            dma((2, 2)),
            dma((2, 2, n_tp - 1)),
            dma((2, 2, n_z - 1)),
            dma((2, n_tp - 1)),
            dma((2, n_fs - 1)),
            dma((2, n_z - 1)),
            dma((2, n_z)),
            dma((2, 2, 2, n_z - 1)),
            dma((2, 2, n_z)),
        ],
        compiler_params=pltpu.CompilerParams(
            collective_id=0, has_side_effects=True, vmem_limit_bytes=VMEM_BYTES
        ),
        name="exchange",
    )(*args)


def update_kernel(
    dirs,
    moments_new,
    in_basis,
    point_basis,
    in_gathered,
    point_gathered,
    in_master,
    point_master,
    in_first_new,
    in_second_new,
    point_first_new,
    point_second_new,
    in_step,
    point_step,
    in_master_new,
    point_master_new,
    in_copy,
    point_copy,
    split,
):
    i = pl.program_id(0)
    f = lax.axis_index("fs")
    rank = split.shape[1] // 2

    @pl.when(i == 0)
    def first_tile():
        for m in range(2):
            whole = dirs[:, m].reshape(rank, split.shape[2])
            high = whole.astype(jnp.bfloat16)
            split[m, :rank] = high
            split[m, rank:] = (whole - high.astype(jnp.float32)).astype(jnp.bfloat16)
        for k, out in enumerate(
            (in_first_new, in_second_new, point_first_new, point_second_new)
        ):
            out[...] = moments_new[k]

    groups = (
        (in_basis, in_gathered, in_master, in_step, in_master_new, in_copy),
        (point_basis, point_gathered, point_master, point_step, point_master_new, point_copy),
    )
    for m, (basis, gathered, master, step, master_new, copy) in enumerate(groups):
        twice = jnp.concatenate([basis[...], basis[...]], axis=1)
        move = -jnp.dot(twice, split[m], preferred_element_type=jnp.float32)
        copy[...] = (gathered[0, 0].astype(jnp.float32) + move).astype(jnp.bfloat16)

        @pl.when(i == f)
        def own_tile():
            step[...] = move
            new = master[...] + move
            master_new[...] = new
            copy[...] = new.astype(jnp.bfloat16)


def update(n_fs, dirs, moments_new, gathered, *args):
    in_basis, in_first, in_master = args[4], args[6], args[10]
    row_count, width = in_master.shape
    rank = in_basis.shape[1]
    f32, bf16 = jnp.float32, jnp.bfloat16

    def fixed(shape):
        return pl.BlockSpec(shape, lambda i: (0,) * len(shape))

    tile = pl.BlockSpec((row_count, rank), lambda i: (i, 0))
    copy_tile = pl.BlockSpec((row_count, width), lambda i: (i, 0))

    def gathered_tile(m):
        return pl.BlockSpec((1, 1, row_count, width), lambda i: (m, i, 0, 0))

    return pl.pallas_call(
        update_kernel,
        grid=(n_fs,),
        out_shape=(
            *(jax.ShapeDtypeStruct(in_first.shape, f32),) * 4,
            *(jax.ShapeDtypeStruct(in_master.shape, f32),) * 4,
            *(jax.ShapeDtypeStruct((row_count * n_fs, width), bf16),) * 2,
        ),
        in_specs=[
            fixed(dirs.shape),
            fixed(moments_new.shape),
            tile,
            tile,
            gathered_tile(0),
            gathered_tile(1),
            fixed(in_master.shape),
            fixed(in_master.shape),
        ],
        out_specs=(
            *(fixed(in_first.shape),) * 4,
            *(fixed(in_master.shape),) * 4,
            copy_tile,
            copy_tile,
        ),
        scratch_shapes=[pltpu.VMEM((2, 2 * rank, width), bf16)],
        compiler_params=pltpu.CompilerParams(vmem_limit_bytes=VMEM_BYTES),
        name="update",
    )(dirs, moments_new, in_basis, args[5], gathered, gathered, in_master, args[11])


def fused_body(*args):
    n_fs, n_tp = lax.axis_size("fs"), lax.axis_size("tp")
    dirs, moments_new, gathered = exchange(n_fs, n_tp, *args)
    return update(n_fs, dirs, moments_new, gathered, *args)


def pick_body(*args):
    n_fs, n_tp = lax.axis_size("fs"), lax.axis_size("tp")
    first = args[6]
    fits = n_fs % 2 == 0 and n_fs > 4 and n_tp > 1
    if fits and first.shape[0] % 16 == 0 and first.shape[1] % 128 == 0:
        return fused_body(*args)
    return body(*args)


def solution(mesh):
    return jax.shard_map(
        pick_body,
        mesh=mesh,
        in_specs=(
            P(("fs", "tp"), None),
            P(("fs", "tp"), None),
            P(("fs", "tp"), None),
            P(("fs", "tp"), None),
            P(),
            P(),
            P("fs", "tp"),
            P("fs", "tp"),
            P("fs", "tp"),
            P("fs", "tp"),
            P("fs", "tp"),
            P("fs", "tp"),
        ),
        out_specs=(
            P("fs", "tp"),
            P("fs", "tp"),
            P("fs", "tp"),
            P("fs", "tp"),
            P("fs", "tp"),
            P("fs", "tp"),
            P("fs", "tp"),
            P("fs", "tp"),
            P(None, "tp"),
            P(None, "tp"),
        ),
        check_vma=False,
    )
```

```python
import functools

import jax
import jax.numpy as jnp
from jax import lax
from jax.experimental import pallas as pl
from jax.experimental.pallas import tpu as pltpu
from jax.sharding import PartitionSpec as P


def low_term(saved, cotangent, basis):
    reduced = jnp.dot(saved, basis, preferred_element_type=jnp.float32).astype(jnp.bfloat16)
    return lax.dot_general(
        reduced, cotangent, (((0,), (0,)), ((), ())), preferred_element_type=jnp.float32
    )


def moments(first, second, grad):
    first_new = 0.8 * first + 0.2 * grad
    second_new = 0.9 * second + 0.1 * grad * grad
    return (first_new, second_new, first_new / (jnp.sqrt(second_new) + 1e-08))


def weight_step(basis, direction, fs_count):
    row_count = basis.shape[0] // fs_count
    rows_here = lax.dynamic_slice_in_dim(basis, lax.axis_index("fs") * row_count, row_count, 0)
    return -jnp.dot(rows_here.astype(jnp.float32), direction, precision=lax.Precision.HIGHEST)


def body(
    in_saved,
    in_cotangent,
    point_saved,
    point_cotangent,
    in_basis,
    point_basis,
    in_first,
    in_second,
    point_first,
    point_second,
    in_master,
    point_master,
):
    fs_count = lax.axis_size("fs")
    in_low = low_term(in_saved, in_cotangent, in_basis)
    point_low = low_term(point_saved, point_cotangent, point_basis)
    rank_rows = in_low.shape[0]
    entries = 1.0 * rank_rows * (in_low.shape[1] + point_low.shape[1])
    part_in, part_point = (
        lax.psum_scatter(in_low, "tp", scatter_dimension=1, tiled=True),
        lax.psum_scatter(point_low, "tp", scatter_dimension=1, tiled=True),
    )
    sum_in, sum_point = lax.psum((part_in, part_point), "fs")
    squares = lax.psum(jnp.sum(sum_in * sum_in) + jnp.sum(sum_point * sum_point), "tp")
    clip_factor = jnp.minimum(1.0, 1.0 / jnp.sqrt(squares / entries + 1e-06))
    previous = (
        lax.all_gather(in_first, "fs", axis=0, tiled=True),
        lax.all_gather(in_second, "fs", axis=0, tiled=True),
        lax.all_gather(point_first, "fs", axis=0, tiled=True),
        lax.all_gather(point_second, "fs", axis=0, tiled=True),
    )
    in_first_all, in_second_all, in_direction = moments(
        previous[0], previous[1], clip_factor * sum_in
    )
    point_first_all, point_second_all, point_direction = moments(
        previous[2], previous[3], clip_factor * sum_point
    )
    row_count = rank_rows // fs_count
    row_start = lax.axis_index("fs") * row_count
    in_first_new = lax.dynamic_slice_in_dim(in_first_all, row_start, row_count, 0)
    in_second_new = lax.dynamic_slice_in_dim(in_second_all, row_start, row_count, 0)
    point_first_new = lax.dynamic_slice_in_dim(point_first_all, row_start, row_count, 0)
    point_second_new = lax.dynamic_slice_in_dim(point_second_all, row_start, row_count, 0)
    in_step = weight_step(in_basis, in_direction, fs_count)
    point_step = weight_step(point_basis, point_direction, fs_count)
    in_master_new = in_master + in_step
    point_master_new = point_master + point_step
    in_copy, point_copy = (
        lax.all_gather(in_master_new.astype(jnp.bfloat16), "fs", axis=0, tiled=True),
        lax.all_gather(point_master_new.astype(jnp.bfloat16), "fs", axis=0, tiled=True),
    )
    return (
        in_first_new,
        in_second_new,
        point_first_new,
        point_second_new,
        in_step,
        point_step,
        in_master_new,
        point_master_new,
        in_copy,
        point_copy,
    )


MESH = pl.DeviceIdType.MESH
HBM = pl.BlockSpec(memory_space=pl.ANY)
VMEM_BYTES = 67_043_328
WHOLE = pl.BlockSpec(memory_space=pltpu.VMEM)


def exchange_kernel(
    n_fs,
    n_tp,
    in_saved,
    in_cot,
    point_saved,
    point_cot,
    in_basis,
    point_basis,
    in_first,
    in_second,
    point_first,
    point_second,
    in_master,
    point_master,
    dirs_out,
    moments_out,
    gathered_out,
    saved,
    cot,
    basis,
    master,
    part,
    mate,
    tp_put,
    tp_got,
    fs_got,
    total,
    dirs,
    old,
    gathered,
    scalars,
    load_sem,
    out_sem,
    mate_sems,
    tp_sems,
    fs_sems,
    tp_scalar_sems,
    fs_scalar_sems,
    dir_sems,
    dir_mate_sems,
    ring_sems,
    ring_mate_sems,
):
    f, t = lax.axis_index("fs"), lax.axis_index("tp")
    z, core = f // 2, f % 2
    n_z = n_fs // 2
    mate_f = f + 1 - 2 * core
    width = in_first.shape[1]
    rows = in_first.shape[0]

    def at_z(step):
        return lax.rem(z + step + n_z, n_z)

    def at_tp(step):
        return lax.rem(t + step + n_tp, n_tp)

    def at_fs(step):
        return lax.rem(f + step + n_fs, n_fs)

    def remote(src, dst, sems, index, device):
        return pltpu.make_async_remote_copy(
            src_ref=src,
            dst_ref=dst,
            send_sem=sems.at[(0, *index)],
            recv_sem=sems.at[(1, *index)],
            device_id=device,
            device_id_type=MESH,
        )

    loads = []
    sources = (
        (in_master, master.at[0]),
        (point_master, master.at[1]),
        (in_basis, basis.at[0]),
        (in_saved, saved.at[0]),
        (in_cot, cot.at[0]),
        (point_basis, basis.at[1]),
        (point_saved, saved.at[1]),
        (point_cot, cot.at[1]),
        (in_first, old.at[0]),
        (in_second, old.at[1]),
        (point_first, old.at[2]),
        (point_second, old.at[3]),
    )
    for k, (src, dst) in enumerate(sources):
        copy = pltpu.make_async_copy(src, dst, load_sem.at[k])
        copy.start()
        loads.append(copy)

    barrier = pltpu.get_barrier_semaphore()
    for step in range(1, n_fs):
        pl.semaphore_signal(barrier, inc=1, device_id=(at_fs(step), t), device_id_type=MESH)
    for step in range(1, n_tp):
        pl.semaphore_signal(barrier, inc=1, device_id=(f, at_tp(step)), device_id_type=MESH)

    sends = []

    def out_copy(m, slot):
        return pltpu.make_async_copy(
            gathered.at[m, slot], gathered_out.at[m, slot], out_sem.at[m, slot]
        )

    def mate_copy(m, slot, sem):
        return remote(
            gathered.at[m, slot], gathered.at[m, slot], ring_mate_sems, (m, sem), (mate_f, t)
        )

    def line_copy(d, m, step):
        slot = 2 * (z - step if d == 0 else z + step) + core
        to = z + 1 if d == 0 else z - 1
        return remote(
            gathered.at[m, slot], gathered.at[m, slot], ring_sems, (d, m, step), (2 * to + core, t)
        )

    def line_sends(d, step):
        if d == 0:
            return (z >= step) & (z + 1 < n_z)
        return (z + step < n_z) & (z >= 1)

    def line_start(m, step):
        for d in range(2):

            @pl.when(line_sends(d, step))
            def start():
                line_copy(d, m, step).start()

    def line_relay(m, step):
        for d in range(2):
            owner = z - 1 - step if d == 0 else z + 1 + step

            @pl.when((owner >= 0) & (owner < n_z))
            def arrived():
                slot = 2 * owner + core
                remote(
                    gathered.at[m, slot], gathered.at[m, slot], ring_sems, (d, m, step), (f, t)
                ).wait_recv()
                if step + 1 < n_z - 1:

                    @pl.when(line_sends(d, step + 1))
                    def onward():
                        line_copy(d, m, step + 1).start()

                mate_copy(m, slot, owner).start()
                out_copy(m, slot).start()

    for m in range(2):
        loads[m].wait()
        gathered[m, f] = master[m].astype(jnp.bfloat16)
    pl.semaphore_wait(barrier, n_fs + n_tp - 2)
    for m in range(2):
        line_start(m, 0)
    for m in range(2):
        mate_copy(m, f, z).start()
        out_copy(m, f).start()
    relays = [(m, step) for step in range(n_z - 1) for m in range(2)]

    for m in range(2):
        for k in range(3):
            loads[2 + 3 * m + k].wait()
        reduced = jnp.dot(saved[m], basis[m], preferred_element_type=jnp.float32).astype(
            jnp.bfloat16
        )
        for k in range(n_tp):
            low = lax.dot_general(
                reduced,
                cot[m, :, k * width : (k + 1) * width],
                (((0,), (0,)), ((), ())),
                preferred_element_type=jnp.float32,
            )
            for g in range(n_fs):
                part[m, g % 2, k, g // 2] = low[g * rows : (g + 1) * rows]
        copy = remote(part.at[m, 1 - core], mate.at[m], mate_sems, (m,), (mate_f, t))
        copy.start()
        sends.append(copy)

    for m in range(2):
        remote(mate.at[m], mate.at[m], mate_sems, (m,), (mate_f, t)).wait_recv()
        for step in range(1, n_tp + 1):
            to = at_tp(step) if step < n_tp else t
            value = part[m, core, to] + mate[m, to]
            if step == n_tp:
                part[m, core, to] = value
            else:
                tp_put[m, step - 1] = value.astype(jnp.bfloat16)
                copy = remote(
                    tp_put.at[m, step - 1], tp_got.at[m, step - 1], tp_sems, (m, step - 1), (f, to)
                )
                copy.start()
                sends.append(copy)
    line_relay(*relays[0])

    for m in range(2):
        for step in range(1, n_tp):
            remote(
                tp_got.at[m, step - 1], tp_got.at[m, step - 1], tp_sems, (m, step - 1), (f, t)
            ).wait_recv()
        for step in range(1, n_z + 1):
            to = at_z(step) if step < n_z else z
            value = part[m, core, t, to]
            for k in range(n_tp - 1):
                value = value + tp_got[m, k, to].astype(jnp.float32)
            total[m, to] = value
            if step < n_z:
                copy = remote(
                    total.at[m, to],
                    fs_got.at[m, step - 1],
                    fs_sems,
                    (m, step - 1),
                    (2 * to + core, t),
                )
                copy.start()
                sends.append(copy)
    line_relay(*relays[1])
    grads = []
    for m in range(2):
        value = total[m, z]
        for step in range(1, n_z):
            remote(
                fs_got.at[m, step - 1], fs_got.at[m, step - 1], fs_sems, (m, step - 1), (f, t)
            ).wait_recv()
            value = value + fs_got[m, step - 1]
        grads.append(value)

    def add_scalars(value, count, base, sems, device):
        scalars[base] = jnp.broadcast_to(value, scalars.shape[1:])
        for step in range(1, count):
            copy = remote(
                scalars.at[base], scalars.at[base + step], sems, (step - 1,), device(step)
            )
            copy.start()
            sends.append(copy)
        result = scalars[base]
        for step in range(1, count):
            slot = scalars.at[base + step]
            remote(slot, slot, sems, (step - 1,), (f, t)).wait_recv()
            result = result + scalars[base + step]
        return result[0:1, 0:1]

    line_relay(*relays[2])
    squares = jnp.sum(grads[0] * grads[0] + grads[1] * grads[1], keepdims=True)
    squares = add_scalars(squares, n_tp, 0, tp_scalar_sems, lambda step: (f, at_tp(step)))
    squares = add_scalars(squares, n_fs, n_tp, fs_scalar_sems, lambda step: (at_fs(step), t))
    line_relay(*relays[3])
    entries = 2.0 * rows * n_fs * width * n_tp
    clip = jnp.minimum(1.0, 1.0 / jnp.sqrt(squares / entries + 1e-06))

    for copy in loads[8:]:
        copy.wait()
    for m in range(2):
        first, second, direction = moments(old[2 * m], old[2 * m + 1], clip * grads[m])
        moments_out[2 * m] = first
        moments_out[2 * m + 1] = second
        dirs[f, m] = direction.astype(jnp.bfloat16)
    for step in range(1, n_z):
        copy = remote(
            dirs.at[f], dirs.at[f], dir_sems, (step - 1,), (2 * at_z(step) + core, t)
        )
        copy.start()
        sends.append(copy)

    def dir_mate(step):
        slot = 2 * at_z(-step) + core
        copy = remote(dirs.at[slot], dirs.at[slot], dir_mate_sems, (step,), (mate_f, t))
        copy.start()
        sends.append(copy)

    dir_mate(0)
    for step in range(1, n_z):
        slot = 2 * at_z(-step) + core
        remote(dirs.at[slot], dirs.at[slot], dir_sems, (step - 1,), (f, t)).wait_recv()
        dir_mate(step)
    for m, step in relays[4:]:
        line_relay(m, step)
    for step in range(n_z):
        slot = 2 * at_z(-step) + 1 - core
        remote(dirs.at[slot], dirs.at[slot], dir_mate_sems, (step,), (f, t)).wait_recv()
    dirs_out[...] = dirs[...]
    for m in range(2):
        for owner in range(n_z):
            slot = 2 * owner + 1 - core
            mate_copy(m, slot, owner).wait_recv()
            out_copy(m, slot).start()
    for copy in sends:
        copy.wait_send()
    for m in range(2):
        for owner in range(n_z):
            mate_copy(m, 2 * owner + core, owner).wait_send()
        for slot in range(n_fs):
            out_copy(m, slot).wait()
        for step in range(n_z - 1):
            for d in range(2):

                @pl.when(line_sends(d, step))
                def sent():
                    line_copy(d, m, step).wait_send()


def exchange(n_fs, n_tp, *args):
    saved, basis, first, master = args[0], args[4], args[6], args[10]
    rows, width = first.shape
    n_z = n_fs // 2
    f32, bf16 = jnp.float32, jnp.bfloat16
    dma = pltpu.SemaphoreType.DMA
    return pl.pallas_call(
        functools.partial(exchange_kernel, n_fs, n_tp),
        out_shape=(
            jax.ShapeDtypeStruct((n_fs, 2, rows, width), bf16),
            jax.ShapeDtypeStruct((4, rows, width), f32),
            jax.ShapeDtypeStruct((2, n_fs, *master.shape), bf16),
        ),
        in_specs=[HBM] * 12,
        out_specs=(WHOLE, WHOLE, HBM),
        scratch_shapes=[
            pltpu.VMEM((2, *saved.shape), bf16),
            pltpu.VMEM((2, *args[1].shape), bf16),
            pltpu.VMEM((2, *basis.shape), bf16),
            pltpu.VMEM((2, *master.shape), f32),
            pltpu.VMEM((2, 2, n_tp, n_z, rows, width), f32),
            pltpu.VMEM((2, n_tp, n_z, rows, width), f32),
            pltpu.VMEM((2, n_tp - 1, n_z, rows, width), bf16),
            pltpu.VMEM((2, n_tp - 1, n_z, rows, width), bf16),
            pltpu.VMEM((2, n_z - 1, rows, width), f32),
            pltpu.VMEM((2, n_z, rows, width), f32),
            pltpu.VMEM((n_fs, 2, rows, width), bf16),
            pltpu.VMEM((4, rows, width), f32),
            pltpu.VMEM((2, n_fs, *master.shape), bf16),
            pltpu.VMEM((n_tp + n_fs, 8, 128), f32),
            dma((12,)),
            dma((2, n_fs)),
            dma((2, 2)),
            dma((2, 2, n_tp - 1)),
            dma((2, 2, n_z - 1)),
            dma((2, n_tp - 1)),
            dma((2, n_fs - 1)),
            dma((2, n_z - 1)),
            dma((2, n_z)),
            dma((2, 2, 2, n_z - 1)),
            dma((2, 2, n_z)),
        ],
        compiler_params=pltpu.CompilerParams(
            collective_id=0, has_side_effects=True, vmem_limit_bytes=VMEM_BYTES
        ),
        name="exchange",
    )(*args)


def update_kernel(
    dirs,
    moments_new,
    in_basis,
    point_basis,
    in_gathered,
    point_gathered,
    in_master,
    point_master,
    in_first_new,
    in_second_new,
    point_first_new,
    point_second_new,
    in_step,
    point_step,
    in_master_new,
    point_master_new,
    in_copy,
    point_copy,
    whole,
):
    i = pl.program_id(0)
    f = lax.axis_index("fs")
    rank = whole.shape[1]

    @pl.when(i == 0)
    def first_tile():
        for m in range(2):
            whole[m] = dirs[:, m].reshape(rank, whole.shape[2])
        for k, out in enumerate(
            (in_first_new, in_second_new, point_first_new, point_second_new)
        ):
            out[...] = moments_new[k]

    groups = (
        (in_basis, in_gathered, in_master, in_step, in_master_new, in_copy),
        (point_basis, point_gathered, point_master, point_step, point_master_new, point_copy),
    )
    for m, (basis, gathered, master, step, master_new, copy) in enumerate(groups):
        move = -jnp.dot(basis[...], whole[m], preferred_element_type=jnp.float32)
        copy[...] = (gathered[0, 0].astype(jnp.float32) + move).astype(jnp.bfloat16)

        @pl.when(i == f)
        def own_tile():
            step[...] = move
            new = master[...] + move
            master_new[...] = new
            copy[...] = new.astype(jnp.bfloat16)


def update(n_fs, dirs, moments_new, gathered, *args):
    in_basis, in_first, in_master = args[4], args[6], args[10]
    row_count, width = in_master.shape
    rank = in_basis.shape[1]
    f32, bf16 = jnp.float32, jnp.bfloat16

    def fixed(shape):
        return pl.BlockSpec(shape, lambda i: (0,) * len(shape))

    tile = pl.BlockSpec((row_count, rank), lambda i: (i, 0))
    copy_tile = pl.BlockSpec((row_count, width), lambda i: (i, 0))

    def gathered_tile(m):
        return pl.BlockSpec((1, 1, row_count, width), lambda i: (m, i, 0, 0))

    return pl.pallas_call(
        update_kernel,
        grid=(n_fs,),
        out_shape=(
            *(jax.ShapeDtypeStruct(in_first.shape, f32),) * 4,
            *(jax.ShapeDtypeStruct(in_master.shape, f32),) * 4,
            *(jax.ShapeDtypeStruct((row_count * n_fs, width), bf16),) * 2,
        ),
        in_specs=[
            fixed(dirs.shape),
            fixed(moments_new.shape),
            tile,
            tile,
            gathered_tile(0),
            gathered_tile(1),
            fixed(in_master.shape),
            fixed(in_master.shape),
        ],
        out_specs=(
            *(fixed(in_first.shape),) * 4,
            *(fixed(in_master.shape),) * 4,
            copy_tile,
            copy_tile,
        ),
        scratch_shapes=[pltpu.VMEM((2, rank, width), bf16)],
        compiler_params=pltpu.CompilerParams(vmem_limit_bytes=VMEM_BYTES),
        name="update",
    )(dirs, moments_new, in_basis, args[5], gathered, gathered, in_master, args[11])


def fused_body(*args):
    n_fs, n_tp = lax.axis_size("fs"), lax.axis_size("tp")
    dirs, moments_new, gathered = exchange(n_fs, n_tp, *args)
    return update(n_fs, dirs, moments_new, gathered, *args)


def pick_body(*args):
    n_fs, n_tp = lax.axis_size("fs"), lax.axis_size("tp")
    first = args[6]
    fits = n_fs % 2 == 0 and n_fs > 4 and n_tp > 1
    if fits and first.shape[0] % 16 == 0 and first.shape[1] % 128 == 0:
        return fused_body(*args)
    return body(*args)


def solution(mesh):
    return jax.shard_map(
        pick_body,
        mesh=mesh,
        in_specs=(
            P(("fs", "tp"), None),
            P(("fs", "tp"), None),
            P(("fs", "tp"), None),
            P(("fs", "tp"), None),
            P(),
            P(),
            P("fs", "tp"),
            P("fs", "tp"),
            P("fs", "tp"),
            P("fs", "tp"),
            P("fs", "tp"),
            P("fs", "tp"),
        ),
        out_specs=(
            P("fs", "tp"),
            P("fs", "tp"),
            P("fs", "tp"),
            P("fs", "tp"),
            P("fs", "tp"),
            P("fs", "tp"),
            P("fs", "tp"),
            P("fs", "tp"),
            P(None, "tp"),
            P(None, "tp"),
        ),
        check_vma=False,
    )
```
